32 devices in a mesh: kv: 8 (over z, y), tp: 4 (over x, core).
Axes of the slice: x: 2, y: 2, z: 4, core: 2. Of those that a mesh axis runs over, the one named last changes fastest.
Arguments:
- piece_tokens: bfloat16 [1024, 4096], P('kv'), may hold values from -6 to 6
- decode_tokens: bfloat16 [8, 4096], P('kv'), may hold values from -6 to 6
- norm_gain: bfloat16 [4096], replicated, may hold values from 0.099609375 to 1.8984375
- w_query: bfloat16 [4096, 2048], P(None, 'tp'), may hold values from -0.09375 to 0.09375
- w_key: bfloat16 [4096, 2048], P(None, 'tp'), may hold values from -0.09375 to 0.09375
- w_value: bfloat16 [4096, 2048], P(None, 'tp'), may hold values from -0.09375 to 0.09375
- score_offset: float32 [16], replicated, may hold values from -14 to -3
- context_length: int32 [1], replicated, may hold values from 4096 to 8192
- prompt_keys: bfloat16 [8192, 2048], P('kv', 'tp'), may hold values from -16 to 16, as said below
- prompt_values: bfloat16 [8192, 2048], P('kv', 'tp'), may hold values from -6 to 6
- decode_keys: bfloat16 [8, 1024, 2048], P('kv', None, 'tp'), may hold values from -6 to 6
- decode_values: bfloat16 [8, 1024, 2048], P('kv', None, 'tp'), may hold values from -6 to 6
- decoding_cache_length: int32 [8], P('kv'), may hold values from 1 to 1024, as said below
- out_gain: bfloat16 [2048], replicated, may hold values from 0.099609375 to 1.8984375
- w_out: bfloat16 [2048, 4096], P(None, 'tp'), may hold values from -0.125 to 0.125
Outputs:
- prompt_piece_output: bfloat16 [1024, 4096], P('kv', 'tp')
- decode_out: bfloat16 [8, 4096], P('kv', 'tp')
- piece_keys: bfloat16 [1024, 2048], P('kv', 'tp')
- piece_values: bfloat16 [1024, 2048], P('kv', 'tp')
- decode_new_keys: bfloat16 [8, 2048], P('kv', 'tp')
- decode_new_values: bfloat16 [8, 2048], P('kv', 'tp')
The draws below stay inside these ranges and needn't reach their ends.
Inputs may be any that keep to these rules, and one draw needn't show every extreme that they name: `prompt_keys`: the largest scale of a block of 1024 positions is up to four times the smallest. `decoding_cache_length`: some sequence has exactly 1024 valid positions.
All inputs are finite; a program needn't handle non-finite values.
Results may differ from the reference program's by a relative error of at most 0.008.
The reference program's roundings to bfloat16 on the way count: a program that leaves them out, or rounds other values in their place, can miss the bound.
Values may be sent and summed in bfloat16 or wider, within the bound.
A program may use at most 128 MiB of HBM per device.

```python
import math
import jax
import jax.numpy as jnp
from jax import lax

D = 4096
HEADS = 16
HEAD = 128
PIECE_DEV = 128
CTX_DEV = 1024
DLEN = 1024
PIECE = 1024
CTX = 8192
DEC = 8


def draw_score_offset(key, part):
    key_offset = jax.random.fold_in(key, 3)
    return jax.random.uniform(key_offset, (HEADS,), jnp.float32, -13.0, -3.0)


def draw_prompt_keys(key, part):
    key_scale, key_values = jax.random.split(jax.random.fold_in(key, 5))
    factors = jnp.exp(jax.random.uniform(key_scale, (CTX // CTX_DEV,), jnp.float32, math.log(0.5), math.log(2.0)))
    values = jnp.clip(jax.random.normal(key_values, (CTX, HEADS * HEAD), jnp.float32), -8.0, 8.0)
    places = jnp.arange(CTX, dtype=jnp.int32) // CTX_DEV
    return (values * factors[places][:, None]).astype(jnp.bfloat16)


def draw_decoding_cache_length(key, part):
    key_lengths, key_spot = jax.random.split(jax.random.fold_in(key, 7))
    lengths = jax.random.randint(key_lengths, (DEC,), 1, DLEN + 1, dtype=jnp.int32)
    spot = jax.random.randint(key_spot, (), 0, DEC, dtype=jnp.int32)
    return jnp.where(jnp.arange(DEC, dtype=jnp.int32) == spot, DLEN, lengths).astype(jnp.int32)


def block_scale(key, dims, shards, low, top_value):
    level = 1.0
    for position, parts in shards:
        steps = jax.random.uniform(jax.random.fold_in(jax.random.fold_in(key, 6), position), (parts,), jnp.float32, low / len(shards), top_value / len(shards))
        level = level * jnp.repeat(jnp.exp(steps), dims[position] // parts).reshape((-1,) + (1,) * (len(dims) - 1 - position))
    return level


def scatter_about(own_key, dims, width, reach, shards=(), kind=jnp.bfloat16):
    values = jax.random.normal(own_key, dims, jnp.float32) * width
    if len(shards) > 0:
        values = block_scale(own_key, dims, shards, -0.22, 0.18) * values
    return jnp.clip(values, min=-reach, max=reach).astype(kind)


def setup_inputs(seed: int = 0) -> dict:
    seeds = jax.random.split(jax.random.key(seed), 16)
    piece_tokens = scatter_about(seeds[0], (PIECE, D), 1.0, 6.0, ((0, 8),))
    decode_tokens = scatter_about(seeds[1], (DEC, D), 1.0, 6.0, ((0, 8),))
    norm_gain = jnp.clip(1.0 + 0.18 * jax.random.normal(seeds[2], (D,), jnp.float32), 0.099609375, 1.8984375).astype(jnp.bfloat16)
    w_query = scatter_about(seeds[3], (D, HEADS * HEAD), D ** -0.5, 0.09375, ((1, 4),))
    w_key = scatter_about(seeds[4], (D, HEADS * HEAD), D ** -0.5, 0.09375, ((1, 4),))
    w_value = scatter_about(seeds[5], (D, HEADS * HEAD), D ** -0.5, 0.09375, ((1, 4),))
    score_offset = draw_score_offset(jax.random.fold_in(seeds[15], 71), 0)
    context_length = jax.random.randint(seeds[7], (1,), CTX // 2, CTX + 1).astype(jnp.int32)
    prompt_keys = draw_prompt_keys(jax.random.fold_in(seeds[15], 71), 0)
    prompt_values = scatter_about(seeds[9], (CTX, HEADS * HEAD), 1.0, 6.0, ((0, 8), (1, 4)))
    decode_keys = scatter_about(seeds[10], (DEC, DLEN, HEADS * HEAD), 1.0, 6.0, ((0, 8), (2, 4)))
    decode_values = scatter_about(seeds[11], (DEC, DLEN, HEADS * HEAD), 1.0, 6.0, ((0, 8), (2, 4)))
    decoding_cache_length = draw_decoding_cache_length(jax.random.fold_in(seeds[15], 71), 0)
    out_gain = jnp.clip(1.0 + 0.18 * jax.random.normal(seeds[13], (HEADS * HEAD,), jnp.float32), 0.099609375, 1.8984375).astype(jnp.bfloat16)
    w_out = scatter_about(seeds[14], (HEADS * HEAD, D), (HEADS * HEAD) ** -0.5, 0.125, ((1, 4),))
    return {"piece_tokens": piece_tokens, "decode_tokens": decode_tokens, "norm_gain": norm_gain, "w_query": w_query, "w_key": w_key, "w_value": w_value, "score_offset": score_offset, "context_length": context_length, "prompt_keys": prompt_keys, "prompt_values": prompt_values, "decode_keys": decode_keys, "decode_values": decode_values, "decoding_cache_length": decoding_cache_length, "out_gain": out_gain, "w_out": w_out}


EPS = 1e-06

def rms_scaled(rows, gain):
    values = rows.astype(jnp.float32)
    inverse = lax.rsqrt(lax.optimization_barrier(jnp.mean(values * values, axis=-1, keepdims=True)) + EPS)
    return values * inverse * gain.astype(jnp.float32)

def block_terms(scores, visible):
    keep = jnp.where(visible, jax.nn.log_sigmoid(-scores), 0.0)
    after = lax.cumsum(keep, axis=scores.ndim - 1, reverse=True) - keep
    weight = jnp.where(visible, jnp.exp(jax.nn.log_sigmoid(scores) + after), 0.0)
    return (weight.astype(jnp.bfloat16), lax.optimization_barrier(jnp.sum(keep, axis=-1)))

def reference(piece_tokens, decode_tokens, norm_gain, w_query, w_key, w_value, score_offset, context_length, prompt_keys, prompt_values, decode_keys, decode_values, decoding_cache_length, out_gain, w_out):
    all_rows = jnp.concatenate([piece_tokens, decode_tokens], axis=0)
    normed_in = rms_scaled(all_rows, norm_gain).astype(jnp.bfloat16)
    queries = jnp.dot(normed_in, w_query, preferred_element_type=jnp.float32).astype(jnp.bfloat16)
    new_keys = jnp.dot(normed_in, w_key, preferred_element_type=jnp.float32).astype(jnp.bfloat16)
    new_values = jnp.dot(normed_in, w_value, preferred_element_type=jnp.float32).astype(jnp.bfloat16)
    score_scale = HEAD ** (-0.5)

    def by_head(matrix, span):
        return matrix.reshape(-1, HEADS, HEAD).transpose(1, 0, 2).reshape(HEADS, -1, span, HEAD)
    piece_queries = queries[:PIECE].reshape(PIECE, HEADS, HEAD).transpose(1, 0, 2)
    cache_k = by_head(prompt_keys, CTX_DEV)
    cached_value_rows = by_head(prompt_values, CTX_DEV)
    piece_k = by_head(new_keys[:PIECE], PIECE_DEV)
    piece_v = by_head(new_values[:PIECE], PIECE_DEV)
    cache_places = jnp.arange(CTX, dtype=jnp.int32).reshape(-1, CTX_DEV)
    valid_mask = cache_places < context_length[0]
    piece_places = jnp.arange(PIECE, dtype=jnp.int32).reshape(-1, PIECE_DEV)

    def per_head(inputs_tuple):
        head_q, head_ck, head_cached_values, head_pk, head_prompt_values, head_offset = inputs_tuple

        def per_block(block_index):
            start = block_index * PIECE_DEV
            query_rows = lax.dynamic_slice_in_dim(head_q, start, PIECE_DEV, 0)
            query_places = start + jnp.arange(PIECE_DEV, dtype=jnp.int32)
            cache_scores = jnp.dot(query_rows, head_ck.reshape(-1, HEAD).T, preferred_element_type=jnp.float32).reshape(PIECE_DEV, -1, CTX_DEV)
            cache_scores = cache_scores * score_scale + head_offset
            cached_weight_rows, cache_total = block_terms(cache_scores, valid_mask[None])
            cached_output = jnp.einsum('vef,efw->vew', cached_weight_rows.astype(jnp.float32), head_cached_values.astype(jnp.float32))
            piece_scores = jnp.dot(query_rows, head_pk.reshape(-1, HEAD).T, preferred_element_type=jnp.float32).reshape(PIECE_DEV, -1, PIECE_DEV)
            piece_scores = piece_scores * score_scale + head_offset
            seen = piece_places[None] < query_places[:, None, None]
            prompt_piece_weight, piece_total = block_terms(piece_scores, seen)
            prompt_piece_output = jnp.einsum('vef,efw->vew', prompt_piece_weight.astype(jnp.float32), head_prompt_values.astype(jnp.float32))
            later_cache = lax.cumsum(cache_total, axis=1, reverse=True) - cache_total
            later_piece = lax.cumsum(piece_total, axis=1, reverse=True) - piece_total
            piece_sum = lax.optimization_barrier(jnp.sum(piece_total, axis=1, keepdims=True))
            mixed = lax.optimization_barrier(jnp.sum(cached_output * jnp.exp(later_cache + piece_sum)[:, :, None], axis=1))
            mixed = mixed + lax.optimization_barrier(jnp.sum(prompt_piece_output * jnp.exp(later_piece)[:, :, None], axis=1))
            return mixed.astype(jnp.bfloat16)
        return lax.map(per_block, jnp.arange(PIECE // PIECE_DEV, dtype=jnp.int32)).reshape(PIECE, HEAD)
    piece_heads = lax.map(per_head, (piece_queries, cache_k, cached_value_rows, piece_k, piece_v, score_offset))
    piece_attention = piece_heads.transpose(1, 0, 2).reshape(PIECE, HEADS * HEAD)
    decode_queries = queries[PIECE:].reshape(DEC, HEADS, HEAD)

    def per_sequence(inputs_tuple):
        seq_q, seq_k, seq_v, seq_length = inputs_tuple
        keys_heads = seq_k.reshape(DLEN, HEADS, HEAD).astype(jnp.float32)
        values_heads = seq_v.reshape(DLEN, HEADS, HEAD).astype(jnp.float32)
        scores = jnp.einsum('hd,khd->hk', seq_q.astype(jnp.float32), keys_heads) * score_scale
        scores = scores + score_offset[:, None]
        seen = jnp.arange(DLEN, dtype=jnp.int32)[None, :] < seq_length
        weight, unused = block_terms(scores, seen)
        result = jnp.einsum('hk,khd->hd', weight.astype(jnp.float32), values_heads)
        return result.astype(jnp.bfloat16).reshape(HEADS * HEAD)
    decode_attention = lax.map(per_sequence, (decode_queries, decode_keys, decode_values, decoding_cache_length))
    attention = jnp.concatenate([piece_attention, decode_attention], axis=0)
    normed_out = rms_scaled(attention, out_gain).astype(jnp.bfloat16)
    outputs = jnp.dot(normed_out, w_out, preferred_element_type=jnp.float32).astype(jnp.bfloat16)
    return (outputs[:PIECE], outputs[PIECE:], new_keys[:PIECE], new_values[:PIECE], new_keys[PIECE:], new_values[PIECE:])
```

```python
import functools

import jax
import jax.numpy as jnp
from jax import lax
from jax.experimental import pallas as pl
from jax.experimental.pallas import tpu as pltpu
from jax.sharding import PartitionSpec as P

HEAD = 128
EPS = 1e-06
HIDDEN = -1e30
MESH = pl.DeviceIdType.MESH


def rms_scaled(rows, gain):
    values = rows.astype(jnp.float32)
    inverse = lax.rsqrt(jnp.mean(values * values, axis=-1, keepdims=True) + EPS)
    return values * inverse * gain.astype(jnp.float32)


def suffix_matrix(size):
    row = lax.broadcasted_iota(jnp.int32, (size, size), 0)
    column = lax.broadcasted_iota(jnp.int32, (size, size), 1)
    return jnp.where(row >= column, 1.0, 0.0).astype(jnp.bfloat16)


def dot_t(a, b):
    return lax.dot_general(a, b, (((1,), (1,)), ((), ())), preferred_element_type=jnp.float32)


def dot(a, b):
    return jnp.dot(a, b, preferred_element_type=jnp.float32)


def suffix_keep(z, suffix):
    keep = -(jnp.maximum(z, 0.0) + jnp.log(1.0 + jnp.exp(-jnp.abs(z))))
    high = keep.astype(jnp.bfloat16)
    low = (keep - high.astype(jnp.float32)).astype(jnp.bfloat16)
    return dot(high, suffix) + dot(low, suffix)


def cached_terms(query, key_of, value_of, bias_of, total_keys, chunk, suffix, scale):
    later = None
    out = None
    for start in reversed(range(0, total_keys, chunk)):
        z = dot_t(query, key_of(start)) * scale + bias_of(start)
        inner = suffix_keep(z, suffix)
        exponent = z + inner if later is None else z + inner + later
        weight = jnp.exp(exponent).astype(jnp.bfloat16)
        part = dot(weight, value_of(start))
        out = part if out is None else out + part
        later = inner[:, 0:1] if later is None else later + inner[:, 0:1]
    return out, later


def attention_kernel(
    n, tp, heads, q_ref, k_ref, v_ref, dq_ref, ck_ref, cv_ref, cbias_ref, off_ref, dk_ref, dv_ref,
    dbias_ref, gain_ref, out_ref, qg, kg, vg, osend, orecv, tsend, trecv, acc, later_s, att, attg,
    q_ss, q_rs, k_ss, k_rs, v_ss, v_rs, o_ss, o_rs, t_ss, t_rs, a_ss, a_rs,
):
    me = lax.axis_index("kv")
    mine = lax.axis_index("tp")
    rows = q_ref.shape[0]
    cache_rows = ck_ref.shape[0]
    seqs, slots = dk_ref.shape[0], dk_ref.shape[1]
    scale = HEAD ** (-0.5)
    chunk = 256 if cache_rows % 256 == 0 else 128

    barrier = pltpu.get_barrier_semaphore()
    for s in range(1, n):
        pl.semaphore_signal(barrier, inc=1, device_id={"kv": lax.rem(me + s, n)}, device_id_type=MESH)
    for s in range(1, tp):
        pl.semaphore_signal(barrier, inc=1, device_id={"tp": lax.rem(mine + s, tp)}, device_id_type=MESH)
    pl.semaphore_wait(barrier, n - 1 + tp - 1)

    def remote(src, dst, ss, rs, peer, axis="kv"):
        return pltpu.make_async_remote_copy(
            src_ref=src, dst_ref=dst, send_sem=ss, recv_sem=rs,
            device_id={axis: peer}, device_id_type=MESH,
        )

    def send_all(src, dst, ss, rs):
        for s in range(1, n):
            peer = lax.rem(me + n - s, n)
            remote(src, dst.at[me], ss.at[s], rs.at[me], peer).start()

    send_all(q_ref, qg, q_ss, q_rs)
    send_all(k_ref, kg, k_ss, k_rs)
    send_all(v_ref, vg, v_ss, v_rs)
    qg[me] = q_ref[...]
    kg[me] = k_ref[...]
    vg[me] = v_ref[...]

    wide = suffix_matrix(chunk)
    width = heads * HEAD
    hrow = lax.broadcasted_iota(jnp.int32, (8, width), 0)
    hcol = lax.broadcasted_iota(jnp.int32, (8, width), 1) // HEAD
    own_head = hrow == hcol
    att[pl.ds(rows, 16), :] = jnp.zeros((16, width), att.dtype)
    dec_rows = jnp.zeros((16, width), jnp.float32)
    for b in range(seqs):
        query = jnp.where(own_head, dq_ref[b : b + 1, :].astype(jnp.float32), 0.0).astype(jnp.bfloat16)
        out, unused = cached_terms(
            query,
            lambda start: dk_ref[b, pl.ds(start, chunk), :],
            lambda start: dv_ref[b, pl.ds(start, chunk), :],
            lambda start: dbias_ref[b, :, pl.ds(start, chunk)],
            slots, chunk, wide, scale,
        )
        row = jnp.sum(jnp.where(own_head, out, 0.0), axis=0, keepdims=True)
        place = lax.broadcasted_iota(jnp.int32, (16, width), 0)
        dec_rows = jnp.where(place == b, row, dec_rows)
    att[pl.ds(rows, 16), :] = dec_rows.astype(att.dtype)

    lane = lax.broadcasted_iota(jnp.int32, (rows, 128), 1)

    def block(s, carry):
        owner = lax.rem(me + s, n)

        @pl.when(s > 0)
        def _():
            remote(q_ref, qg.at[owner], q_ss.at[s], q_rs.at[owner], owner).wait_recv()

        totals = jnp.zeros((rows, 128), jnp.float32)
        for h in range(heads):
            cols = pl.ds(h * HEAD, HEAD)
            out, total = cached_terms(
                qg[owner, :, cols],
                lambda start: ck_ref[pl.ds(start, chunk), cols],
                lambda start: cv_ref[pl.ds(start, chunk), cols],
                lambda start: cbias_ref[h : h + 1, pl.ds(start, chunk)],
                cache_rows, chunk, wide, scale,
            )
            osend[owner, :, cols] = out.astype(jnp.bfloat16)
            totals = jnp.where(lane == h, total, totals)
        tsend[owner] = jnp.transpose(totals)[0:8, :]

        @pl.when(s > 0)
        def _():
            place = pl.ds(pl.multiple_of(me * 8, 8), 8)
            remote(tsend.at[owner], trecv.at[place], t_ss.at[s], t_rs.at[me], owner).start()
            remote(osend.at[owner], orecv.at[me], o_ss.at[s], o_rs.at[me], owner).start()

        return carry

    lax.fori_loop(0, n, block, 0)
    orecv[me] = osend[me]
    trecv[pl.ds(pl.multiple_of(me * 8, 8), 8), :] = tsend[me]

    for s in range(1, n):
        peer = lax.rem(me + s, n)
        remote(k_ref, kg.at[peer], k_ss.at[s], k_rs.at[peer], peer).wait()
        remote(v_ref, vg.at[peer], v_ss.at[s], v_rs.at[peer], peer).wait()
        remote(q_ref, qg.at[peer], q_ss.at[s], q_rs.at[peer], peer).wait_send()

    narrow = suffix_matrix(rows)
    qrow = lax.broadcasted_iota(jnp.int32, (rows, rows), 0)
    kcol = lax.broadcasted_iota(jnp.int32, (rows, rows), 1)
    acc[...] = jnp.zeros_like(acc)

    def piece(step, later):
        j = n - 1 - step
        seen = (j * rows + kcol) < (me * rows + qrow)
        nexts = []
        for h in range(heads):
            cols = pl.ds(h * HEAD, HEAD)
            z = dot_t(q_ref[:, cols], kg[j, :, cols]) * scale + off_ref[h : h + 1, 0:1]
            z = jnp.where(seen, z, HIDDEN)
            inner = suffix_keep(z, narrow)
            weight = jnp.exp(z + inner).astype(jnp.bfloat16)
            acc[:, cols] += dot(weight, vg[j, :, cols]) * jnp.exp(later[h])
            nexts.append(later[h] + inner[:, 0:1])
        return tuple(nexts)

    piece_total = lax.fori_loop(
        0, n, piece, tuple(jnp.zeros((rows, 1), jnp.float32) for _ in range(heads))
    )

    for s in range(1, n):
        peer = lax.rem(me + s, n)
        place = pl.ds(pl.multiple_of(peer * 8, 8), 8)
        remote(tsend.at[peer], trecv.at[place], t_ss.at[s], t_rs.at[peer], peer).wait()
        remote(osend.at[peer], orecv.at[peer], o_ss.at[s], o_rs.at[peer], peer).wait()

    run = jnp.zeros((8, 128), jnp.float32)
    later_s[...] = jnp.zeros_like(later_s)
    for c in reversed(range(n)):
        later_s[c * 8 : c * 8 + 8, :] = run
        run = run + trecv[c * 8 : c * 8 + 8, :]
    factors = [
        jnp.exp(jnp.transpose(later_s[g * 128 : g * 128 + 128, :]))
        for g in range(later_s.shape[0] // 128)
    ]
    for h in range(heads):
        cols = pl.ds(h * HEAD, HEAD)
        mixed = jnp.zeros((rows, HEAD), jnp.float32)
        for c in range(n):
            group, spot = divmod(c * 8 + h, 128)
            mixed += orecv[c, :, cols].astype(jnp.float32) * factors[group][:, spot : spot + 1]
        mixed = mixed * jnp.exp(piece_total[h]) + acc[:, cols]
        att[pl.ds(0, rows), cols] = mixed.astype(att.dtype)

    for s in range(1, tp):
        peer = lax.rem(mine + s, tp)
        remote(att, attg.at[mine], a_ss.at[s], a_rs.at[mine], peer, "tp").start()
    attg[mine] = att[...]
    for s in range(1, tp):
        peer = lax.rem(mine + s, tp)
        remote(att, attg.at[peer], a_ss.at[s], a_rs.at[peer], peer, "tp").wait()
    square = jnp.zeros((att.shape[0], 1), jnp.float32)
    for t in range(tp):
        values = attg[t].astype(jnp.float32)
        square += jnp.sum(values * values, axis=-1, keepdims=True)
    inverse = lax.rsqrt(square / (tp * width) + EPS)
    for t in range(tp):
        cols = pl.ds(t * width, width)
        gain = gain_ref[0:1, cols].astype(jnp.float32)
        out_ref[:, cols] = (attg[t].astype(jnp.float32) * inverse * gain).astype(out_ref.dtype)


def body(
    piece_tokens, decode_tokens, norm_gain, w_query, w_key, w_value, score_offset, context_length,
    prompt_keys, prompt_values, decode_keys, decode_values, decoding_cache_length, out_gain, w_out,
):
    n, tp = lax.axis_size("kv"), lax.axis_size("tp")
    width = w_query.shape[1]
    heads = width // HEAD
    offset = lax.dynamic_slice_in_dim(score_offset, lax.axis_index("tp") * heads, heads)
    offset = jnp.pad(offset, (0, 8 - heads))
    rows = piece_tokens.shape[0]
    all_rows = jnp.concatenate([piece_tokens, decode_tokens], axis=0)
    normed_in = rms_scaled(all_rows, norm_gain).astype(jnp.bfloat16)
    queries = jnp.dot(normed_in, w_query, preferred_element_type=jnp.float32).astype(jnp.bfloat16)
    new_keys = jnp.dot(normed_in, w_key, preferred_element_type=jnp.float32).astype(jnp.bfloat16)
    new_values = jnp.dot(normed_in, w_value, preferred_element_type=jnp.float32).astype(
        jnp.bfloat16
    )
    cache_rows = prompt_keys.shape[0]
    seqs, slots = decode_keys.shape[:2]
    places = lax.axis_index("kv") * cache_rows + jnp.arange(cache_rows, dtype=jnp.int32)
    cache_bias = jnp.where(places[None, :] < context_length[0], offset[:, None], HIDDEN)
    spots = jnp.arange(slots, dtype=jnp.int32)[None, None, :]
    decode_bias = jnp.where(
        spots < decoding_cache_length[:, None, None], offset[None, :, None], HIDDEN
    )
    wide_offset = jnp.broadcast_to(offset[:, None], (8, 128))
    trows = -(-n * 8 // 128) * 128
    vmem = pl.BlockSpec(memory_space=pltpu.VMEM)
    dma = pltpu.SemaphoreType.DMA
    block = pltpu.VMEM((n, rows, width), jnp.bfloat16)
    normed_out = pl.pallas_call(
        functools.partial(attention_kernel, n, tp, heads),
        out_shape=jax.ShapeDtypeStruct((rows + 16, tp * width), jnp.bfloat16),
        in_specs=[vmem] * 12,
        out_specs=vmem,
        scratch_shapes=[
            block, block, block, block, block,
            pltpu.VMEM((n, 8, 128), jnp.float32),
            pltpu.VMEM((trows, 128), jnp.float32),
            pltpu.VMEM((rows, width), jnp.float32),
            pltpu.VMEM((trows, 128), jnp.float32),
            pltpu.VMEM((rows + 16, width), jnp.bfloat16),
            pltpu.VMEM((tp, rows + 16, width), jnp.bfloat16),
        ] + [dma((n,)) for _ in range(10)] + [dma((tp,)), dma((tp,))],
        compiler_params=pltpu.CompilerParams(
            collective_id=0, has_side_effects=True, vmem_limit_bytes=56 * 1024 * 1024
        ),
        name="attend",
    )(
        queries[:rows], new_keys[:rows], new_values[:rows], queries[rows:], prompt_keys,
        prompt_values, cache_bias, wide_offset, decode_keys, decode_values, decode_bias,
        out_gain[None, :],
    )
    outputs = jnp.dot(normed_out, w_out, preferred_element_type=jnp.float32).astype(jnp.bfloat16)
    return (
        outputs[:rows],
        outputs[rows : rows + seqs],
        new_keys[:rows],
        new_values[:rows],
        new_keys[rows:],
        new_values[rows:],
    )


def solution(mesh):
    in_specs = (
        P("kv", None),
        P("kv", None),
        P(),
        P(None, "tp"),
        P(None, "tp"),
        P(None, "tp"),
        P(),
        P(),
        P("kv", "tp"),
        P("kv", "tp"),
        P("kv", None, "tp"),
        P("kv", None, "tp"),
        P("kv"),
        P(),
        P(None, "tp"),
    )
    out_specs = (
        P("kv", "tp"),
        P("kv", "tp"),
        P("kv", "tp"),
        P("kv", "tp"),
        P("kv", "tp"),
        P("kv", "tp"),
    )
    return jax.shard_map(body, mesh=mesh, in_specs=in_specs, out_specs=out_specs, check_vma=False)
```

```python
import functools

import jax
import jax.numpy as jnp
from jax import lax
from jax.experimental import pallas as pl
from jax.experimental.pallas import tpu as pltpu
from jax.sharding import PartitionSpec as P

HEAD = 128
EPS = 1e-06
HIDDEN = -1e30
MESH = pl.DeviceIdType.MESH


def rms_scaled(rows, gain):
    values = rows.astype(jnp.float32)
    inverse = lax.rsqrt(jnp.mean(values * values, axis=-1, keepdims=True) + EPS)
    return values * inverse * gain.astype(jnp.float32)


def suffix_matrix(size):
    row = lax.broadcasted_iota(jnp.int32, (size, size), 0)
    column = lax.broadcasted_iota(jnp.int32, (size, size), 1)
    return jnp.where(row >= column, 1.0, 0.0).astype(jnp.bfloat16)


def dot_t(a, b):
    return lax.dot_general(a, b, (((1,), (1,)), ((), ())), preferred_element_type=jnp.float32)


def dot(a, b):
    return jnp.dot(a, b, preferred_element_type=jnp.float32)


def suffix_keep(z, suffix):
    keep = -(jnp.maximum(z, 0.0) + jnp.log(1.0 + jnp.exp(-jnp.abs(z))))
    high = keep.astype(jnp.bfloat16)
    low = (keep - high.astype(jnp.float32)).astype(jnp.bfloat16)
    return dot(high, suffix) + dot(low, suffix)


def cached_terms(query, key_of, value_of, bias_of, total_keys, chunk, suffix, scale):
    later = None
    out = None
    for start in reversed(range(0, total_keys, chunk)):
        z = dot_t(query, key_of(start)) * scale + bias_of(start)
        inner = suffix_keep(z, suffix)
        exponent = z + inner if later is None else z + inner + later
        weight = jnp.exp(exponent).astype(jnp.bfloat16)
        part = dot(weight, value_of(start))
        out = part if out is None else out + part
        later = inner[:, 0:1] if later is None else later + inner[:, 0:1]
    return out, later


def attention_kernel(
    n, tp, heads, q_ref, k_ref, v_ref, dq_ref, ck_ref, cv_ref, cbias_ref, off_ref, dk_ref, dv_ref,
    dbias_ref, gain_ref, out_ref, qg, osend, orecv, psend, precv, tsend, trecv, ptot, later_s, att, attg,
    q_ss, q_rs, p_ss, p_rs, o_ss, o_rs, t_ss, t_rs, a_ss, a_rs,
):
    me = lax.axis_index("kv")
    mine = lax.axis_index("tp")
    rows = q_ref.shape[0]
    cache_rows = ck_ref.shape[0]
    seqs, slots = dk_ref.shape[0], dk_ref.shape[1]
    scale = HEAD ** (-0.5)
    chunk = 256 if cache_rows % 256 == 0 else 128

    barrier = pltpu.get_barrier_semaphore()
    for s in range(1, n):
        pl.semaphore_signal(barrier, inc=1, device_id={"kv": lax.rem(me + s, n)}, device_id_type=MESH)
    for s in range(1, tp):
        pl.semaphore_signal(barrier, inc=1, device_id={"tp": lax.rem(mine + s, tp)}, device_id_type=MESH)
    pl.semaphore_wait(barrier, n - 1 + tp - 1)

    def remote(src, dst, ss, rs, peer, axis="kv"):
        return pltpu.make_async_remote_copy(
            src_ref=src, dst_ref=dst, send_sem=ss, recv_sem=rs,
            device_id={axis: peer}, device_id_type=MESH,
        )

    def send_all(src, dst, ss, rs):
        for s in range(1, n):
            peer = lax.rem(me + n - s, n)
            remote(src, dst.at[me], ss.at[s], rs.at[me], peer).start()

    send_all(q_ref, qg, q_ss, q_rs)
    qg[me] = q_ref[...]

    wide = suffix_matrix(chunk)
    width = heads * HEAD
    hrow = lax.broadcasted_iota(jnp.int32, (8, width), 0)
    hcol = lax.broadcasted_iota(jnp.int32, (8, width), 1) // HEAD
    own_head = hrow == hcol
    att[pl.ds(rows, 16), :] = jnp.zeros((16, width), att.dtype)
    dec_rows = jnp.zeros((16, width), jnp.float32)
    for b in range(seqs):
        query = jnp.where(own_head, dq_ref[b : b + 1, :].astype(jnp.float32), 0.0).astype(jnp.bfloat16)
        out, unused = cached_terms(
            query,
            lambda start: dk_ref[b, pl.ds(start, chunk), :],
            lambda start: dv_ref[b, pl.ds(start, chunk), :],
            lambda start: dbias_ref[b, :, pl.ds(start, chunk)],
            slots, chunk, wide, scale,
        )
        row = jnp.sum(jnp.where(own_head, out, 0.0), axis=0, keepdims=True)
        place = lax.broadcasted_iota(jnp.int32, (16, width), 0)
        dec_rows = jnp.where(place == b, row, dec_rows)
    att[pl.ds(rows, 16), :] = dec_rows.astype(att.dtype)

    lane = lax.broadcasted_iota(jnp.int32, (rows, 128), 1)
    narrow = suffix_matrix(rows)
    qrow = lax.broadcasted_iota(jnp.int32, (rows, rows), 0)
    kcol = lax.broadcasted_iota(jnp.int32, (rows, rows), 1)
    for c in range(n):

        @pl.when(c > me)
        def _():
            precv[c] = jnp.zeros((rows, width), jnp.bfloat16)


    def block(s, carry):
        owner = lax.rem(me + s, n)

        @pl.when(s > 0)
        def _():
            remote(q_ref, qg.at[owner], q_ss.at[s], q_rs.at[owner], owner).wait_recv()

        totals = jnp.zeros((rows, 128), jnp.float32)
        for h in range(heads):
            cols = pl.ds(h * HEAD, HEAD)
            out, total = cached_terms(
                qg[owner, :, cols],
                lambda start: ck_ref[pl.ds(start, chunk), cols],
                lambda start: cv_ref[pl.ds(start, chunk), cols],
                lambda start: cbias_ref[h : h + 1, pl.ds(start, chunk)],
                cache_rows, chunk, wide, scale,
            )
            osend[owner, :, cols] = out.astype(jnp.bfloat16)
            totals = jnp.where(lane == h, total, totals)
        ptot[...] = totals

        @pl.when(owner >= me)
        def _():
            seen = (me * rows + kcol) < (owner * rows + qrow)
            totals = ptot[...]
            for h in range(heads):
                cols = pl.ds(h * HEAD, HEAD)
                z = dot_t(qg[owner, :, cols], k_ref[:, cols]) * scale + off_ref[h : h + 1, 0:1]
                z = jnp.where(seen, z, HIDDEN)
                inner = suffix_keep(z, narrow)
                weight = jnp.exp(z + inner).astype(jnp.bfloat16)
                psend[owner, :, cols] = dot(weight, v_ref[:, cols]).astype(jnp.bfloat16)
                totals = jnp.where(lane == heads + h, inner[:, 0:1], totals)
            ptot[...] = totals

        tsend[owner] = jnp.transpose(ptot[...])[0:8, :]

        @pl.when(s > 0)
        def _():
            place = pl.ds(pl.multiple_of(me * 8, 8), 8)
            remote(tsend.at[owner], trecv.at[place], t_ss.at[s], t_rs.at[me], owner).start()
            remote(osend.at[owner], orecv.at[me], o_ss.at[s], o_rs.at[me], owner).start()

        @pl.when(owner > me)
        def _():
            remote(psend.at[owner], precv.at[me], p_ss.at[s], p_rs.at[me], owner).start()

        return carry

    lax.fori_loop(0, n, block, 0)
    orecv[me] = osend[me]
    precv[me] = psend[me]
    trecv[pl.ds(pl.multiple_of(me * 8, 8), 8), :] = tsend[me]

    for s in range(1, n):
        peer = lax.rem(me + s, n)
        place = pl.ds(pl.multiple_of(peer * 8, 8), 8)
        remote(tsend.at[peer], trecv.at[place], t_ss.at[s], t_rs.at[peer], peer).wait()
        remote(osend.at[peer], orecv.at[peer], o_ss.at[s], o_rs.at[peer], peer).wait()
        remote(q_ref, qg.at[peer], q_ss.at[s], q_rs.at[peer], peer).wait_send()
        pieces = remote(psend.at[peer], precv.at[peer], p_ss.at[s], p_rs.at[peer], peer)

        @pl.when(peer > me)
        def _():
            pieces.wait_send()

        @pl.when(peer < me)
        def _():
            pieces.wait_recv()

    run = jnp.zeros((8, 128), jnp.float32)
    later_s[...] = jnp.zeros_like(later_s)
    for c in reversed(range(n)):
        later_s[c * 8 : c * 8 + 8, :] = run
        run = run + trecv[c * 8 : c * 8 + 8, :]
    later_s[n * 8 : n * 8 + 8, :] = run
    factors = [
        jnp.exp(jnp.transpose(later_s[g * 128 : g * 128 + 128, :]))
        for g in range(later_s.shape[0] // 128)
    ]

    def factor(c, row):
        group, spot = divmod(c * 8 + row, 128)
        return factors[group][:, spot : spot + 1]

    for h in range(heads):
        cols = pl.ds(h * HEAD, HEAD)
        mixed = jnp.zeros((rows, HEAD), jnp.float32)
        pieces = jnp.zeros((rows, HEAD), jnp.float32)
        for c in range(n):
            mixed += orecv[c, :, cols].astype(jnp.float32) * factor(c, h)
            pieces += precv[c, :, cols].astype(jnp.float32) * factor(c, heads + h)
        mixed = mixed * factor(n, heads + h) + pieces
        att[pl.ds(0, rows), cols] = mixed.astype(att.dtype)

    for s in range(1, tp):
        peer = lax.rem(mine + s, tp)
        remote(att, attg.at[mine], a_ss.at[s], a_rs.at[mine], peer, "tp").start()
    attg[mine] = att[...]
    for s in range(1, tp):
        peer = lax.rem(mine + s, tp)
        remote(att, attg.at[peer], a_ss.at[s], a_rs.at[peer], peer, "tp").wait()
    square = jnp.zeros((att.shape[0], 1), jnp.float32)
    for t in range(tp):
        values = attg[t].astype(jnp.float32)
        square += jnp.sum(values * values, axis=-1, keepdims=True)
    inverse = lax.rsqrt(square / (tp * width) + EPS)
    for t in range(tp):
        cols = pl.ds(t * width, width)
        gain = gain_ref[0:1, cols].astype(jnp.float32)
        out_ref[:, cols] = (attg[t].astype(jnp.float32) * inverse * gain).astype(out_ref.dtype)


def body(
    piece_tokens, decode_tokens, norm_gain, w_query, w_key, w_value, score_offset, context_length,
    prompt_keys, prompt_values, decode_keys, decode_values, decoding_cache_length, out_gain, w_out,
):
    n, tp = lax.axis_size("kv"), lax.axis_size("tp")
    width = w_query.shape[1]
    heads = width // HEAD
    offset = lax.dynamic_slice_in_dim(score_offset, lax.axis_index("tp") * heads, heads)
    offset = jnp.pad(offset, (0, 8 - heads))
    rows = piece_tokens.shape[0]
    all_rows = jnp.concatenate([piece_tokens, decode_tokens], axis=0)
    normed_in = rms_scaled(all_rows, norm_gain).astype(jnp.bfloat16)
    queries = jnp.dot(normed_in, w_query, preferred_element_type=jnp.float32).astype(jnp.bfloat16)
    new_keys = jnp.dot(normed_in, w_key, preferred_element_type=jnp.float32).astype(jnp.bfloat16)
    new_values = jnp.dot(normed_in, w_value, preferred_element_type=jnp.float32).astype(
        jnp.bfloat16
    )
    cache_rows = prompt_keys.shape[0]
    seqs, slots = decode_keys.shape[:2]
    places = lax.axis_index("kv") * cache_rows + jnp.arange(cache_rows, dtype=jnp.int32)
    cache_bias = jnp.where(places[None, :] < context_length[0], offset[:, None], HIDDEN)
    spots = jnp.arange(slots, dtype=jnp.int32)[None, None, :]
    decode_bias = jnp.where(
        spots < decoding_cache_length[:, None, None], offset[None, :, None], HIDDEN
    )
    wide_offset = jnp.broadcast_to(offset[:, None], (8, 128))
    trows = -(-(n + 1) * 8 // 128) * 128
    vmem = pl.BlockSpec(memory_space=pltpu.VMEM)
    dma = pltpu.SemaphoreType.DMA
    block = pltpu.VMEM((n, rows, width), jnp.bfloat16)
    normed_out = pl.pallas_call(
        functools.partial(attention_kernel, n, tp, heads),
        out_shape=jax.ShapeDtypeStruct((rows + 16, tp * width), jnp.bfloat16),
        in_specs=[vmem] * 12,
        out_specs=vmem,
        scratch_shapes=[
            block, block, block, block, block,
            pltpu.VMEM((n, 8, 128), jnp.float32),
            pltpu.VMEM((trows, 128), jnp.float32),
            pltpu.VMEM((rows, 128), jnp.float32),
            pltpu.VMEM((trows, 128), jnp.float32),
            pltpu.VMEM((rows + 16, width), jnp.bfloat16),
            pltpu.VMEM((tp, rows + 16, width), jnp.bfloat16),
        ] + [dma((n,)) for _ in range(8)] + [dma((tp,)), dma((tp,))],
        compiler_params=pltpu.CompilerParams(
            collective_id=0, has_side_effects=True, vmem_limit_bytes=56 * 1024 * 1024
        ),
        name="attend",
    )(
        queries[:rows], new_keys[:rows], new_values[:rows], queries[rows:], prompt_keys,
        prompt_values, cache_bias, wide_offset, decode_keys, decode_values, decode_bias,
        out_gain[None, :],
    )
    outputs = jnp.dot(normed_out, w_out, preferred_element_type=jnp.float32).astype(jnp.bfloat16)
    return (
        outputs[:rows],
        outputs[rows : rows + seqs],
        new_keys[:rows],
        new_values[:rows],
        new_keys[rows:],
        new_values[rows:],
    )


def solution(mesh):
    in_specs = (
        P("kv", None),
        P("kv", None),
        P(),
        P(None, "tp"),
        P(None, "tp"),
        P(None, "tp"),
        P(),
        P(),
        P("kv", "tp"),
        P("kv", "tp"),
        P("kv", None, "tp"),
        P("kv", None, "tp"),
        P("kv"),
        P(),
        P(None, "tp"),
    )
    out_specs = (
        P("kv", "tp"),
        P("kv", "tp"),
        P("kv", "tp"),
        P("kv", "tp"),
        P("kv", "tp"),
        P("kv", "tp"),
    )
    return jax.shard_map(body, mesh=mesh, in_specs=in_specs, out_specs=out_specs, check_vma=False)
```
